256 devices in a mesh: sp: 64 (over z, y, core), tp: 4 (over x).
Axes of the slice: x: 4, y: 4, z: 8, core: 2. Of those that a mesh axis runs over, the one named last changes fastest.
Arguments:
- out_grad: bfloat16 [12288, 2048], P('sp'), may hold values from -16 to 16
- routes: int32 [12288, 2], P('sp'), may hold values from 0 to 63, all different within a row; in each aligned block of 192 rows (0 to 191, 192 to 383, ...) at most 12 rows name the same one
- route_weight: float32 [12288, 2], P('sp'), may hold values from 0.3 to 1.5
- expert_rows: bfloat16 [64, 64, 12, 2048], P(None, 'sp'), may hold values from -6 to 6
- gate_weight: bfloat16 [64, 2048, 1024], P('sp', None, 'tp'), may hold values from -0.125 to 0.125
- up_weight: bfloat16 [64, 2048, 1024], P('sp', None, 'tp'), may hold values from -0.125 to 0.125
- down_weight: bfloat16 [64, 1024, 2048], P('sp', 'tp'), may hold values from -0.1875 to 0.1875
- conv_input: bfloat16 [12288, 1024], P('sp', 'tp'), may hold values from -6 to 6
- out_gate: bfloat16 [12288, 1024], P('sp', 'tp'), may hold values from -6 to 6
- in_gate: bfloat16 [12288, 1024], P('sp', 'tp'), may hold values from -6 to 6
- taps: float32 [3, 1024], P(None, 'tp'), may hold values from -3 to 3
- out_weight: bfloat16 [2048, 1024], P(None, 'tp'), may hold values from -0.1875 to 0.1875
Outputs:
- gate_grad: bfloat16 [64, 2048, 1024], P('sp', None, 'tp')
- up_grad: bfloat16 [64, 2048, 1024], P('sp', None, 'tp')
- down_grad: bfloat16 [64, 1024, 2048], P('sp', 'tp')
- mid_grad: bfloat16 [12288, 2048], P('sp', 'tp')
- out_weight_grad: float32 [2048, 1024], P('sp', 'tp')
- input_grad: bfloat16 [12288, 1024], P('sp', 'tp')
- out_gate_grad: bfloat16 [12288, 1024], P('sp', 'tp')
- in_gate_grad: bfloat16 [12288, 1024], P('sp', 'tp')
The draws below stay inside these ranges and needn't reach their ends.
Inputs may be any that keep to these rules, and one draw needn't show every extreme that they name: `routes`: each token names 2 different experts; within each aligned block of 192 tokens no expert is named by more than 12 tokens, a bound that some block reaches.
All inputs are finite; a program needn't handle non-finite values.
Results may differ from the reference program's by a relative error of at most 0.014.
Values may be sent and summed in bfloat16 or wider, within the bound.
No kernel may reach another device: no remote copies, remote signals or barrier semaphores. Data moves between devices by JAX's collectives and lax.ppermute only.
A program may use at most 64 MiB of HBM per device.

```python
import math
import jax
import jax.numpy as jnp
import numpy as np
from jax import lax

D = 2048
CHANNELS = 1024
FF = 1024
TOP_K = 2
TAPS = 3
EXP_DEV = 1
TOK_DEV = 192
EXPERTS = 64
TOKENS = 12288
CAP = 12
N_SP = 64
N_TP = 4


def with_spikes(result, key, source, target, parts, factor):
    def block_of(dim):
        return (jnp.arange(result.shape[dim]) // (result.shape[dim] // parts)).reshape((-1,) + (1,) * (result.ndim - 1 - dim))

    near = jax.random.permutation(key, parts)[block_of(target)]
    far = (block_of(target) + parts // 2) % parts
    return jnp.where((block_of(source) == near) | (block_of(source) == far), factor * result, result)


def levels(stream_key, shape, shards, least, top_value):
    def one(position, parts):
        heights = jax.random.uniform(jax.random.fold_in(jax.random.fold_in(stream_key, 6), position), (parts,), jnp.float32, least / len(shards), top_value / len(shards))
        return jnp.repeat(jnp.exp(heights), shape[position] // parts).reshape((-1,) + (1,) * (len(shape) - position - 1))

    loudness = one(*shards[0])
    for cut in shards[1:]:
        loudness = loudness * one(*cut)
    return loudness


def shared_out(stream_key, own, number, rows, count, top, bound, slope):
    ranking = jax.random.permutation(stream_key, count)
    packed, usual = load_shares(count, rows * top, bound, slope, True), load_shares(count, rows * top, bound, slope, False)
    places = jnp.arange(count)

    def named(tallies, offset_by):
        used = int((tallies > 0).sum())
        fixed = max(1, used // 4)
        shifted = fixed + (places - fixed + offset_by * (used - fixed)) % max(1, count - fixed)
        return jnp.zeros((count,), jnp.int32).at[ranking[jnp.where(places < fixed, places, shifted)]].set(jnp.asarray(tallies, jnp.int32))

    tallies = jnp.where(number % 4 == 0, named(packed, number // 4), named(usual, number - number // 4 - 1))
    mixed = jax.random.permutation(jax.random.fold_in(own, 3), count)
    giver, receiver = mixed[0:count // 2 * 2:2], mixed[1:count // 2 * 2:2]
    margin = jnp.minimum(tallies[giver] - 1, bound - tallies[receiver]) // 2
    margin = jnp.where((giver == ranking[0]) | (receiver == ranking[0]) | (tallies[receiver] == 0), 0, jnp.maximum(margin, 0))
    shifted = jax.random.randint(jax.random.fold_in(own, 4), (count // 2,), 0, 1 << 20) % (margin + 1)
    tallies = tallies.at[giver].add(-shifted).at[receiver].add(shifted)
    members = jnp.searchsorted(jnp.cumsum(tallies), jnp.arange(rows * top), side="right").astype(jnp.int32)
    listing = members.reshape(top, rows).T
    listing = listing[jax.random.permutation(jax.random.fold_in(own, 1), rows)]
    offset_by = jax.random.randint(jax.random.fold_in(own, 2), (rows, 1), 0, top)
    return jnp.take_along_axis(listing, (jnp.arange(top)[None, :] + offset_by) % top, axis=1)


def load_shares(amount, total, reach, lean, full):
    loads = [(1 << 20) // math.isqrt(grade ** lean) + 1 for grade in range(1, amount + 1)]
    largest = reach if full else min(reach, max(-(-total // amount), total * loads[0] // sum(loads)))
    least = 1 if total - largest >= amount - 1 else 0
    holding, surplus = [largest] + [least] * (amount - 1), total - largest - least * (amount - 1)
    while surplus > 0:
        free = [i for i in range(1, amount) if holding[i] < largest] or [i for i in range(1, amount) if holding[i] < reach]
        mass, remaining = sum([loads[i] for i in free]), surplus
        for i in free:
            addition = min(reach - holding[i], max(1, remaining * loads[i] // mass), surplus)
            holding[i] = holding[i] + addition
            surplus = surplus - addition
    return np.array(holding)


def scatter_about(key, shape, scale, limit, cuts=(), kind=jnp.bfloat16):
    factor_of = levels(key, shape, cuts, -0.22, 0.18) if cuts else 1.0
    result = jax.random.normal(key, shape, jnp.float32) * scale * factor_of
    return jnp.minimum(jnp.maximum(result, -limit), limit).astype(kind)


def gaussian_with(stream_key, extent, spread, bound, pieces, heavy, held_as=jnp.bfloat16):
    entries = spread * jax.random.normal(stream_key, extent, jnp.float32)
    if pieces:
        entries = entries * levels(stream_key, extent, pieces, -0.22, 0.18)
    return jnp.clip(with_spikes(entries, jax.random.fold_in(stream_key, 3), *heavy), -bound, bound).astype(held_as)


def setup_inputs(seed: int = 0) -> dict:
    streams_of = jax.random.split(jax.random.key(seed), 13)
    out_grad = gaussian_with(streams_of[0], (TOKENS, D), 1.0, 16.0, ((0, 64),), (0, 1, 64, 4.0))
    routes_keys = jax.random.split(jax.random.fold_in(streams_of[1], 1), TOKENS // TOK_DEV)
    routes_turns = jax.random.permutation(jax.random.fold_in(streams_of[1], 3), TOKENS // TOK_DEV)
    routes = jax.vmap(lambda own, number: shared_out(jax.random.fold_in(streams_of[1], 2), own, number, TOK_DEV, EXPERTS, TOP_K, CAP, 1))(routes_keys, routes_turns).reshape((TOKENS, TOP_K))
    route_weight = jnp.clip(0.3 + 1.2 * jax.random.uniform(streams_of[2], (TOKENS, TOP_K), jnp.float32) ** levels(streams_of[2], (TOKENS, TOP_K), ((0, 64),), -0.2, 0.2), 0.3, 1.5)
    expert_rows = scatter_about(streams_of[3], (EXPERTS // EXP_DEV, EXPERTS, CAP, D), 1.0, 6.0, ((1, 64),))
    gate_weight = scatter_about(streams_of[4], (EXPERTS, D, FF), D ** -0.5, 0.125, ((0, 64), (2, 4)))
    up_weight = scatter_about(streams_of[5], (EXPERTS, D, FF), D ** -0.5, 0.125, ((0, 64), (2, 4)))
    down_weight = scatter_about(streams_of[6], (EXPERTS, FF, D), FF ** -0.5, 0.1875, ((0, 64), (1, 4)))
    conv_input = scatter_about(streams_of[7], (TOKENS, CHANNELS), 1.0, 6.0, ((0, 64), (1, 4)))
    out_gate = scatter_about(streams_of[8], (TOKENS, CHANNELS), 1.0, 6.0, ((0, 64), (1, 4)))
    in_gate = scatter_about(streams_of[9], (TOKENS, CHANNELS), 1.0, 6.0, ((0, 64), (1, 4)))
    taps = scatter_about(streams_of[10], (TAPS, CHANNELS), 0.6, 3.0, ((1, 4),), jnp.float32)
    out_weight = scatter_about(streams_of[11], (D, CHANNELS), CHANNELS ** -0.5, 0.1875, ((1, 4),))
    return {"out_grad": out_grad, "routes": routes, "route_weight": route_weight, "expert_rows": expert_rows, "gate_weight": gate_weight, "up_weight": up_weight, "down_weight": down_weight, "conv_input": conv_input, "out_gate": out_gate, "in_gate": in_gate, "taps": taps, "out_weight": out_weight}


def slot_layout(routes):
    flat = routes.reshape(N_SP, TOK_DEV * TOP_K)
    onehot = (flat[:, :, None] == jnp.arange(EXPERTS, dtype=jnp.int32)[None, None, :]).astype(jnp.int32)
    before = jnp.cumsum(onehot, axis=1) - onehot
    place = jnp.sum(before * onehot, axis=2).astype(jnp.int32)
    source = jnp.broadcast_to(jnp.arange(N_SP, dtype=jnp.int32)[:, None], flat.shape)
    return flat, place, source


def one_expert(operands):
    rows, grads, w_gate, w_up, w_down = operands
    rows = rows.reshape(-1, D)
    grads = grads.reshape(-1, D)
    gate = jnp.dot(rows, w_gate, preferred_element_type=jnp.float32)
    up = jnp.dot(rows, w_up, preferred_element_type=jnp.float32)
    sig = jax.nn.sigmoid(gate)
    act = (gate * sig * up).astype(jnp.bfloat16)
    act_grad = jnp.dot(grads, w_down.T, preferred_element_type=jnp.float32)
    up_part = (act_grad * gate * sig).astype(jnp.bfloat16)
    gate_part = (act_grad * up * sig * (1.0 + gate * (1.0 - sig))).astype(jnp.bfloat16)
    down_g = jnp.dot(act.T, grads, preferred_element_type=jnp.float32).astype(jnp.bfloat16)
    gate_g = jnp.dot(rows.T, gate_part, preferred_element_type=jnp.float32).astype(jnp.bfloat16)
    up_g = jnp.dot(rows.T, up_part, preferred_element_type=jnp.float32).astype(jnp.bfloat16)
    group = FF // N_TP
    total = jnp.zeros((rows.shape[0], D), jnp.float32)
    for index in range(N_TP):
        lower = index * group
        upper = lower + group
        part = jnp.dot(gate_part[:, lower:upper], w_gate[:, lower:upper].T, preferred_element_type=jnp.float32)
        part = part + jnp.dot(up_part[:, lower:upper], w_up[:, lower:upper].T, preferred_element_type=jnp.float32)
        rounded = lax.optimization_barrier(part.astype(jnp.bfloat16))
        total = total + rounded.astype(jnp.float32)
    row_grad = total.astype(jnp.bfloat16).reshape(N_SP, CAP, D)
    return gate_g, up_g, down_g, row_grad


def reference(out_grad, routes, route_weight, expert_rows, gate_weight, up_weight, down_weight,
              conv_input, out_gate, in_gate, taps, out_weight):
    flat, place, source = slot_layout(routes)
    slot_grad = (route_weight[:, :, None] * out_grad[:, None, :].astype(jnp.float32)).astype(jnp.bfloat16)
    slot_grad = slot_grad.reshape(N_SP, TOK_DEV * TOP_K, D)
    expert_grads = jnp.zeros((N_SP, EXPERTS, CAP, D), jnp.bfloat16).at[source, flat, place].set(slot_grad)
    rows_by_expert = jnp.moveaxis(expert_rows, 1, 0)
    grads_by_expert = jnp.moveaxis(expert_grads, 1, 0)
    gate_grad, up_grad, down_grad, row_grad = lax.map(
        one_expert, (rows_by_expert, grads_by_expert, gate_weight, up_weight, down_weight))
    picked = row_grad[flat, source, place].astype(jnp.float32)
    picked = picked.reshape(TOKENS, TOP_K, D).sum(axis=1)
    mid_grad = (out_grad.astype(jnp.float32) + picked).astype(jnp.bfloat16)
    mixed = in_gate.astype(jnp.float32) * conv_input.astype(jnp.float32)
    padded = jnp.concatenate([jnp.zeros((TAPS - 1, CHANNELS), jnp.float32), mixed], axis=0)
    conv = jnp.zeros_like(mixed)
    for tap in range(TAPS):
        conv = conv + taps[tap][None, :] * padded[TAPS - 1 - tap:TAPS - 1 - tap + TOKENS]
    gated = (out_gate.astype(jnp.float32) * conv).astype(jnp.bfloat16)
    out_weight_grad = jnp.dot(mid_grad.T, gated, preferred_element_type=jnp.float32)
    gated_grad = jnp.dot(mid_grad, out_weight, preferred_element_type=jnp.float32)
    out_gate_grad = (gated_grad * conv).astype(jnp.bfloat16)
    conv_grad = gated_grad * out_gate.astype(jnp.float32)
    after = jnp.concatenate([conv_grad, jnp.zeros((TAPS - 1, CHANNELS), jnp.float32)], axis=0)
    mixed_grad = jnp.zeros_like(conv_grad)
    for tap in range(TAPS):
        mixed_grad = mixed_grad + taps[tap][None, :] * after[tap:tap + TOKENS]
    input_grad = (mixed_grad * in_gate.astype(jnp.float32)).astype(jnp.bfloat16)
    in_gate_grad = (mixed_grad * conv_input.astype(jnp.float32)).astype(jnp.bfloat16)
    return (gate_grad, up_grad, down_grad, mid_grad, out_weight_grad,
            input_grad, out_gate_grad, in_gate_grad)
```

```python
import jax
import jax.numpy as jnp
from jax import lax
from jax.sharding import PartitionSpec as P

F32 = jnp.float32
BF16 = jnp.bfloat16


def mm(a, b, contract):
    return lax.dot_general(a, b, ((contract[0], contract[1]), ((), ())), preferred_element_type=F32)


def turn(shard, by):
    peers = lax.axis_size("tp")
    return lax.ppermute(shard, "tp", [(i, (i + by) % peers) for i in range(peers)])


def passed_along(shard, axis, by):
    peers = lax.axis_size(axis)
    pairs = [(i, i + by) for i in range(peers) if 0 <= i + by < peers]
    return lax.ppermute(shard, axis, pairs)


def after(value, *others):
    return lax.optimization_barrier((value, *others))[0]


def gathered(own):
    half = own.shape[0] // 2
    left = turn(own, 1)
    right = turn(own, -1)
    far_a = turn(left[:half], 1)
    far_b = turn(right[half:], -1)
    return own, left, right, jnp.concatenate([far_a, far_b], axis=0)


def on_device(
    out_grad,
    routes,
    route_weight,
    expert_rows,
    gate_weight,
    up_weight,
    down_weight,
    conv_input,
    out_gate,
    in_gate,
    taps,
    out_weight,
):
    groups = lax.axis_size("tp")
    member = lax.axis_index("tp")
    sources = lax.axis_size("sp")
    tok_rows, width = out_grad.shape
    slots = expert_rows.shape[2]
    share = width // groups
    portion = slots // groups
    experts = sources
    hidden = gate_weight.shape[2]
    rows = slots * sources

    w_down = gathered(down_weight[0])

    ids = jnp.arange(experts, dtype=jnp.int32)
    first = routes[:, 0][None, :] == ids[:, None]
    second = routes[:, 1][None, :] == ids[:, None]
    named = first | second
    earlier = (
        lax.broadcasted_iota(jnp.int32, (tok_rows, tok_rows), 0)
        < lax.broadcasted_iota(jnp.int32, (tok_rows, tok_rows), 1)
    ).astype(BF16)
    place = mm(named.astype(BF16), earlier, ((1,), (0,))).astype(jnp.int32)
    place = jnp.where(named, place, -1)
    weight = jnp.where(first, route_weight[:, 0][None, :], 0.0) + jnp.where(
        second, route_weight[:, 1][None, :], 0.0
    )
    mine = member * portion + jnp.arange(portion, dtype=jnp.int32)
    chosen = place[:, None, :] == mine[None, :, None]
    slot_weight = jnp.sum(jnp.where(chosen, weight[:, None, :], 0.0), axis=2)
    piece = mm(
        chosen.astype(BF16).reshape(experts * portion, tok_rows), out_grad, ((1,), (0,))
    )
    piece = (piece * slot_weight.reshape(experts * portion, 1)).astype(BF16)
    piece = piece.reshape(experts, portion * width // 128, 128)
    arrived = lax.all_to_all(piece, "sp", split_axis=0, concat_axis=0, tiled=True)
    grads = (
        arrived.reshape(sources, portion, width)
        .transpose(1, 0, 2)
        .reshape(portion * sources, width)
    )

    inputs = expert_rows[:, 0].transpose(1, 0, 2).reshape(rows, width)
    gate_w, up_w = gate_weight[0], up_weight[0]
    gate = mm(inputs, gate_w, ((1,), (0,)))
    up = mm(inputs, up_w, ((1,), (0,)))
    sig = jax.nn.sigmoid(gate)
    act = (gate * sig * up).astype(BF16)
    both_w = jnp.concatenate([gate_w, up_w], axis=1)

    partial = [mm(grads, w, ((1,), (1,))).astype(BF16) for w in w_down]
    from_far = turn(partial[3], 2)
    from_left = turn(partial[2], 1)
    from_right = turn(partial[1], -1)
    around = [partial[0], from_right, from_far, from_left]
    wrapped = jnp.concatenate(around + around, axis=0)
    block = portion * sources
    act_grad = lax.dynamic_slice_in_dim(
        wrapped, (groups - member) * block, groups * block, 0
    ).astype(F32)
    up_part = (act_grad * gate * sig).astype(BF16)
    gate_part = (act_grad * up * sig * (1.0 + gate * (1.0 - sig))).astype(BF16)
    parts = jnp.concatenate([gate_part, up_part], axis=1)

    def row_part(by):
        which = lax.rem(member + by, groups)
        w = lax.dynamic_slice_in_dim(both_w, which * share, share, 0)
        return mm(parts, w, ((1,), (1,)))

    half = rows // 2
    far = row_part(2).astype(BF16)
    far_a = turn(far[:half], 1)
    far_b = turn(far[half:], -1)
    next_part = row_part(1).astype(BF16)
    prev_part = row_part(3).astype(BF16)
    left_b = turn(next_part[half:], 1)
    right_a = turn(prev_part[:half], -1)
    own = row_part(0)
    left_a = turn((next_part[:half].astype(F32) + far_a.astype(F32)).astype(BF16), 1)
    right_b = turn((prev_part[half:].astype(F32) + far_b.astype(F32)).astype(BF16), -1)
    summed = jnp.concatenate(
        [
            own[:half] + left_a.astype(F32) + right_a.astype(F32),
            own[half:] + left_b.astype(F32) + right_b.astype(F32),
        ],
        axis=0,
    ).astype(BF16)
    leaving = summed.reshape(slots, sources, share).transpose(1, 0, 2)
    leaving = leaving.reshape(sources, slots * share // 128, 128)
    returned = lax.all_to_all(leaving, "sp", split_axis=0, concat_axis=0, tiled=True)
    returned = returned.reshape(experts * slots, share)

    every = gathered(after(grads, summed))
    act_wrapped = act.reshape(groups, block, hidden)
    act_wrapped = jnp.concatenate([act_wrapped, act_wrapped], axis=0)
    act_rel = lax.dynamic_slice_in_dim(act_wrapped, member, groups, 0)
    down_grad = mm(act_rel[0], every[0], ((0,), (0,)))
    down_grad = down_grad + mm(act_rel[3], every[1], ((0,), (0,)))
    down_grad = down_grad + mm(act_rel[1], every[2], ((0,), (0,)))
    down_grad = down_grad + mm(act_rel[2], every[3], ((0,), (0,)))
    down_grad = down_grad.astype(BF16)[None]
    gate_grad = mm(inputs, gate_part, ((0,), (0,))).astype(BF16)[None]
    up_grad = mm(inputs, up_part, ((0,), (0,))).astype(BF16)[None]

    slot_ids = jnp.arange(slots, dtype=jnp.int32)
    pick = (place[:, None, :] == slot_ids[None, :, None]).astype(BF16)
    picked = mm(pick.reshape(experts * slots, tok_rows), returned, ((0,), (0,)))
    own_cols = lax.dynamic_slice_in_dim(out_grad, member * share, share, 1).astype(F32)
    mid_grad = (own_cols + picked).astype(BF16)
    mid_whole = lax.all_gather(mid_grad, "tp", axis=1, tiled=True)

    reach = taps.shape[0] - 1
    mixed = in_gate.astype(F32) * conv_input.astype(F32)
    prior_mixed = passed_along(mixed[tok_rows - reach :], "sp", 1)
    extended = jnp.concatenate([prior_mixed, mixed], axis=0)
    conv = jnp.zeros_like(mixed)
    for tap in range(reach + 1):
        conv = conv + taps[tap][None, :] * extended[reach - tap : reach - tap + tok_rows]
    gated = (out_gate.astype(F32) * conv).astype(BF16)
    weight_part = mm(mid_whole, gated, ((0,), (0,))).astype(BF16)
    pieces = lax.all_to_all(
        weight_part.reshape(sources, width // sources, -1), "sp", 0, 0, tiled=True
    )
    out_weight_grad = jnp.sum(pieces.astype(F32), axis=0)
    gated_grad = mm(mid_whole, out_weight, ((1,), (0,)))
    out_gate_grad = (gated_grad * conv).astype(BF16)
    conv_grad = gated_grad * out_gate.astype(F32)
    later = passed_along(conv_grad[:reach], "sp", -1)
    following = jnp.concatenate([conv_grad, later], axis=0)
    mixed_grad = jnp.zeros_like(conv_grad)
    for tap in range(reach + 1):
        mixed_grad = mixed_grad + taps[tap][None, :] * following[tap : tap + tok_rows]
    input_grad = (mixed_grad * in_gate.astype(F32)).astype(BF16)
    in_gate_grad = (mixed_grad * conv_input.astype(F32)).astype(BF16)
    return (
        gate_grad,
        up_grad,
        down_grad,
        mid_grad,
        out_weight_grad,
        input_grad,
        out_gate_grad,
        in_gate_grad,
    )


def solution(mesh):
    in_specs = (
        P("sp", None),
        P("sp", None),
        P("sp", None),
        P(None, "sp", None, None),
        P("sp", None, "tp"),
        P("sp", None, "tp"),
        P("sp", "tp", None),
        P("sp", "tp"),
        P("sp", "tp"),
        P("sp", "tp"),
        P(None, "tp"),
        P(None, "tp"),
    )
    out_specs = (
        P("sp", None, "tp"),
        P("sp", None, "tp"),
        P("sp", "tp", None),
        P("sp", "tp"),
        P("sp", "tp"),
        P("sp", "tp"),
        P("sp", "tp"),
        P("sp", "tp"),
    )
    return jax.shard_map(
        on_device, mesh=mesh, in_specs=in_specs, out_specs=out_specs, check_vma=False
    )
```

```python
import jax
import jax.numpy as jnp
from jax import lax
from jax.experimental import pallas as pl
from jax.experimental.pallas import tpu as pltpu
from jax.sharding import PartitionSpec as P


F32 = jnp.float32
BF16 = jnp.bfloat16


def mm(a, b, contract):
    return lax.dot_general(a, b, ((contract[0], contract[1]), ((), ())), preferred_element_type=F32)


def slot_hits(routes_ref, slots, rows):
    tokens = routes_ref.shape[1]
    row = lax.broadcasted_iota(jnp.int32, (rows, tokens), 0)
    expert = lax.shift_right_logical(row * ((1 << 17) // slots + 1), 17)
    slot = row - expert * slots
    first = routes_ref[0:1, :] == expert
    second = routes_ref[1:2, :] == expert
    named = jnp.where(first | second, 1.0, 0.0)
    sooner = lax.broadcasted_iota(jnp.int32, (tokens, tokens), 0)
    later = lax.broadcasted_iota(jnp.int32, (tokens, tokens), 1)
    order = jnp.where(sooner < later, 1.0, 0.0).astype(BF16)
    place = mm(named.astype(BF16), order, ((1,), (0,)))
    return first, named, place, slot.astype(F32)


def send_kernel(
    first_ref, routes_hbm, weight_hbm, tokens_hbm,
    out_ref, wide_ref, routes_ref, weight_ref, tokens_ref, sems,
):
    loads = [
        pltpu.make_async_copy(routes_hbm, routes_ref, sems.at[0]),
        pltpu.make_async_copy(weight_hbm, weight_ref, sems.at[1]),
        pltpu.make_async_copy(tokens_hbm, tokens_ref, sems.at[2]),
    ]
    for load in loads:
        load.start()
    loads[0].wait()
    loads[1].wait()
    rows = out_ref.shape[0] // (tokens_ref.shape[1] // 128)
    portion = rows // 64
    first, named, place, slot = slot_hits(routes_ref, portion, rows)
    base = first_ref[0].astype(F32)
    hit = jnp.where(place == slot + base, named, 0.0)
    weight = hit * jnp.where(first, weight_ref[0:1, :], weight_ref[1:2, :])
    factor = jnp.sum(weight, axis=1, keepdims=True)
    loads[2].wait()
    picked = mm(hit.astype(BF16), tokens_ref[...], ((1,), (0,))) * factor
    lanes = tokens_ref.shape[1] // 128
    for g in range(lanes):
        wide_ref[pl.ds(g, rows, stride=lanes), :] = picked[:, g * 128 : (g + 1) * 128]
    out_ref[...] = wide_ref[...].astype(BF16)


def arrive_kernel(
    arrived_hbm, w0_hbm, w1_hbm, w2_hbm, w3a_hbm, w3b_hbm,
    rows_ref, p0, p1, p2, p3, wide_ref, arrived_ref, w0, w1, w2, w3, sems,
):
    half = w3a_hbm.shape[0]
    loads = [
        pltpu.make_async_copy(arrived_hbm, arrived_ref, sems.at[0]),
        pltpu.make_async_copy(w3a_hbm, w3.at[pl.ds(0, half), :], sems.at[1]),
        pltpu.make_async_copy(w3b_hbm, w3.at[pl.ds(half, half), :], sems.at[2]),
        pltpu.make_async_copy(w2_hbm, w2, sems.at[3]),
        pltpu.make_async_copy(w1_hbm, w1, sems.at[4]),
        pltpu.make_async_copy(w0_hbm, w0, sems.at[5]),
    ]
    for load in loads:
        load.start()
    loads[0].wait()
    wide_ref[...] = arrived_ref[...].astype(F32)
    sources = 64
    per = arrived_ref.shape[0] // sources
    lanes = rows_ref.shape[1] // 128
    for i in range(per // lanes):
        for g in range(lanes):
            rows_ref[i * sources : (i + 1) * sources, g * 128 : (g + 1) * 128] = wide_ref[
                pl.ds(i * lanes + g, sources, stride=per), :
            ].astype(BF16)
    loads[1].wait()
    loads[2].wait()
    p3[...] = mm(rows_ref[...], w3[...], ((1,), (1,))).astype(BF16)
    for load, w, p in ((loads[3], w2, p2), (loads[4], w1, p1), (loads[5], w0, p0)):
        load.wait()
        p[...] = mm(rows_ref[...], w[...], ((1,), (1,))).astype(BF16)


def row_block(gate_part, up_part, gate_ref, up_ref, which, share):
    span = pl.ds(pl.multiple_of(which * share, share), share)
    block = mm(gate_part, gate_ref[span, :], ((1,), (1,)))
    return block + mm(up_part, up_ref[span, :], ((1,), (1,)))


def parts_kernel(
    member_ref, own, right, far, left, up_of, gate_of, gate_ref, up_ref,
    gate_part, up_part, far_a, far_b,
):
    member = member_ref[0]
    groups = 4
    block = own.shape[0]
    for r, piece in enumerate((own, right, far, left)):
        span = pl.ds(pl.multiple_of(lax.rem(member + r, groups) * block, block), block)
        grad = piece[...].astype(F32)
        up_part[span, :] = (grad * up_of[span, :]).astype(BF16)
        gate_part[span, :] = (grad * gate_of[span, :]).astype(BF16)
    share = far_a.shape[1]
    half = far_a.shape[0]
    which = lax.rem(member + 2, groups)
    part = row_block(gate_part[...], up_part[...], gate_ref, up_ref, which, share).astype(BF16)
    far_a[...] = part[:half]
    far_b[...] = part[half:]


def blocks_kernel(
    member_ref, gate_part, up_part, gate_ref, up_ref,
    next_a, next_b, prev_a, prev_b, own,
):
    member = member_ref[0]
    half, share = next_a.shape
    for by, a, b in ((1, next_a, next_b), (3, prev_a, prev_b)):
        which = lax.rem(member + by, 4)
        part = row_block(gate_part[...], up_part[...], gate_ref, up_ref, which, share)
        a[...] = part[:half].astype(BF16)
        b[...] = part[half:].astype(BF16)
    own[...] = row_block(gate_part[...], up_part[...], gate_ref, up_ref, member, share)


def leave_kernel(own, left_a, right_a, left_b, right_b, out_ref, wide_ref):
    sources = 64
    half, share = left_a.shape
    lanes = share // 128
    per = out_ref.shape[0] // sources
    for p in range(per // lanes):
        left, right = (left_a, right_a) if p * sources < half else (left_b, right_b)
        at = p * sources
        here = at if at < half else at - half
        rows = own[at : at + sources, :]
        rows = rows + left[here : here + sources, :].astype(F32)
        rows = rows + right[here : here + sources, :].astype(F32)
        for g in range(lanes):
            wide_ref[pl.ds(p * lanes + g, sources, stride=per), :] = rows[
                :, g * 128 : (g + 1) * 128
            ]
    out_ref[...] = wide_ref[...].astype(BF16)


def return_kernel(
    core_ref, routes_ref, returned_ref, own_ref, gated_ref,
    mid_ref, sent_ref, kept_ref, wide_ref,
):
    share = mid_ref.shape[1]
    lanes = share // 128
    columns = returned_ref.shape[0] // lanes
    wide_ref[...] = returned_ref[...].astype(F32)
    _, named, place, slot = slot_hits(routes_ref, columns // 64, columns)
    hit = jnp.where(place == slot, named, 0.0).T.astype(BF16)
    for g in range(lanes):
        rows = wide_ref[pl.ds(g, columns, stride=lanes), :].astype(BF16)
        picked = mm(hit, rows, ((1,), (0,)))
        own = own_ref[:, g * 128 : (g + 1) * 128].astype(F32)
        mid_ref[:, g * 128 : (g + 1) * 128] = (own + picked).astype(BF16)
    side = share // 2
    core = core_ref[0]
    for ref, which in ((sent_ref, 1 - core), (kept_ref, core)):
        columns_t = mid_ref[:, pl.ds(pl.multiple_of(which * side, side), side)].T
        for r in range(gated_ref.shape[0]):
            part = mm(columns_t, gated_ref[r], ((1,), (0,)))
            ref[r] = part.astype(ref.dtype)


def down_kernel(act, g0, g1, g2, g3a, g3b, out_ref):
    half = g3a.shape[0]
    total = mm(act[0].T, g0[...], ((1,), (0,)))
    total = total + mm(act[3].T, g1[...], ((1,), (0,)))
    total = total + mm(act[1].T, g2[...], ((1,), (0,)))
    total = total + mm(act[2, :half].T, g3a[...], ((1,), (0,)))
    total = total + mm(act[2, half:].T, g3b[...], ((1,), (0,)))
    out_ref[...] = total.astype(BF16)


def weights_kernel(x_ref, gate_part, up_part, gate_ref, up_ref):
    x = x_ref[...].T
    gate_ref[...] = mm(x, gate_part[...], ((1,), (0,))).astype(BF16)
    up_ref[...] = mm(x, up_part[...], ((1,), (0,))).astype(BF16)


def weight_grads(inputs, gate_part, up_part):
    rows, width = inputs.shape
    hidden = gate_part.shape[1]
    tile = 512
    whole = pl.BlockSpec((rows, hidden), lambda i: (0, 0))
    out = pl.BlockSpec((tile, hidden), lambda i: (i, 0))
    return pl.pallas_call(
        weights_kernel,
        grid=(width // tile,),
        out_shape=[jax.ShapeDtypeStruct((width, hidden), BF16)] * 2,
        in_specs=[pl.BlockSpec((rows, tile), lambda i: (0, i)), whole, whole],
        out_specs=[out, out],
        compiler_params=pltpu.CompilerParams(vmem_limit_bytes=40 << 20),
        name="weights",
    )(inputs, gate_part, up_part)


def call(kernel, outs, scratch, *args, there=False):
    smem = pl.BlockSpec(memory_space=pltpu.SMEM)
    vmem = pl.BlockSpec(memory_space=pltpu.VMEM)
    hbm = pl.BlockSpec(memory_space=pl.ANY)
    return pl.pallas_call(
        kernel,
        out_shape=[jax.ShapeDtypeStruct(*o) for o in outs],
        in_specs=[smem if a.ndim == 1 else hbm if there else vmem for a in args],
        out_specs=[vmem] * len(outs),
        scratch_shapes=scratch,
        compiler_params=pltpu.CompilerParams(vmem_limit_bytes=40 << 20),
    )(*args)


def turn(shard, by):
    peers = lax.axis_size("tp")
    return lax.ppermute(shard, "tp", [(i, (i + by) % peers) for i in range(peers)])


def passed_along(shard, axis, by):
    peers = lax.axis_size(axis)
    pairs = [(i, i + by) for i in range(peers) if 0 <= i + by < peers]
    return lax.ppermute(shard, axis, pairs)


def after(value, *others):
    return lax.optimization_barrier((value, *others))[0]


def gathered(own):
    half = own.shape[0] // 2
    left = turn(own, 1)
    right = turn(own, -1)
    passed_a = left[:half]
    far_a = turn(passed_a, 1)
    passed_b = right[half:]
    far_b = turn(passed_b, -1)
    return (own, left, right, far_a, far_b), (passed_a, passed_b)


def on_device(
    out_grad,
    routes,
    route_weight,
    expert_rows,
    gate_weight,
    up_weight,
    down_weight,
    conv_input,
    out_gate,
    in_gate,
    taps,
    out_weight,
):
    groups = lax.axis_size("tp")
    member = lax.axis_index("tp")
    sources = lax.axis_size("sp")
    tok_rows, width = out_grad.shape
    slots = expert_rows.shape[2]
    share = width // groups
    portion = slots // groups
    experts = sources
    hidden = gate_weight.shape[2]
    rows = slots * sources

    w_down, passed = gathered(down_weight[0])

    packed = portion * width // 128
    (piece,) = call(
        send_kernel,
        [((experts * packed, 128), BF16)],
        [
            pltpu.VMEM((experts * packed, 128), F32),
            pltpu.VMEM(routes.T.shape, jnp.int32),
            pltpu.VMEM(routes.T.shape, F32),
            pltpu.VMEM(out_grad.shape, BF16),
            pltpu.SemaphoreType.DMA((3,)),
        ],
        (member * portion)[None],
        routes.T,
        route_weight.T,
        out_grad,
        there=True,
    )
    arrived = lax.all_to_all(
        piece.reshape(experts, packed, 128), "sp", split_axis=0, concat_axis=0, tiled=True
    )

    in_gate, conv_input, out_gate, early_grad, out_weight = lax.optimization_barrier(
        (in_gate, conv_input, out_gate, out_grad, out_weight, piece, *passed)
    )[:5]
    own_cols = lax.dynamic_slice_in_dim(early_grad, member * share, share, 1)
    reach = taps.shape[0] - 1
    mixed = in_gate.astype(F32) * conv_input.astype(F32)
    prior_mixed = passed_along(mixed[tok_rows - reach :], "sp", 1)
    extended = jnp.concatenate([prior_mixed, mixed], axis=0)
    conv = jnp.zeros_like(mixed)
    for tap in range(reach + 1):
        conv = conv + taps[tap][None, :] * extended[reach - tap : reach - tap + tok_rows]
    gated = (out_gate.astype(F32) * conv).astype(BF16)
    gated_all = jnp.stack([gated, turn(gated, -1), turn(gated, 2), turn(gated, 1)])
    out_weight_twice = jnp.concatenate([out_weight, out_weight], axis=0)
    out_weight_rel = lax.dynamic_slice_in_dim(out_weight_twice, member * share, width, 0)

    inputs = expert_rows[:, 0].transpose(1, 0, 2).reshape(rows, width)
    inputs = after(inputs, *passed)
    gate_w, up_w = gate_weight[0], up_weight[0]
    gate = mm(inputs, gate_w, ((1,), (0,)))
    up = mm(inputs, up_w, ((1,), (0,)))
    sig = jax.nn.sigmoid(gate)
    act = (gate * sig * up).astype(BF16)
    up_of = gate * sig
    gate_of = up * sig * (1.0 + gate * (1.0 - sig))
    act_twice = act.reshape(groups, rows // groups, hidden)
    act_twice = jnp.concatenate([act_twice, act_twice], axis=0)
    act_rel = lax.dynamic_slice_in_dim(act_twice, member, groups, 0)
    (
        arrived, up_of, gate_of, act_rel, gated_all, out_weight_rel, conv, own_cols
    ) = lax.optimization_barrier(
        (arrived, up_of, gate_of, act_rel, gated_all, out_weight_rel, conv, own_cols)
    )

    block = portion * sources
    grads, *partial = call(
        arrive_kernel,
        [((block, width), BF16)] + [((block, hidden), BF16)] * 4,
        [
            pltpu.VMEM((sources * packed, 128), F32),
            pltpu.VMEM((sources * packed, 128), BF16),
            *[pltpu.VMEM((hidden, width), BF16)] * 4,
            pltpu.SemaphoreType.DMA((6,)),
        ],
        arrived.reshape(sources * packed, 128),
        *w_down,
        there=True,
    )
    from_far = turn(partial[3], 2)
    from_left = turn(partial[2], 1)
    from_right = turn(partial[1], -1)
    half = rows // 2
    gate_part, up_part, far_a, far_b = call(
        parts_kernel,
        [((rows, hidden), BF16)] * 2 + [((half, share), BF16)] * 2,
        [],
        member[None],
        partial[0],
        from_right,
        from_far,
        from_left,
        up_of,
        gate_of,
        gate_w,
        up_w,
    )
    far_a = turn(far_a, 1)
    far_b = turn(far_b, -1)
    next_a, next_b, prev_a, prev_b, own = call(
        blocks_kernel,
        [((half, share), BF16)] * 4 + [((rows, share), F32)],
        [],
        member[None],
        gate_part,
        up_part,
        gate_w,
        up_w,
    )
    left_b = turn(next_b, 1)
    right_a = turn(prev_a, -1)
    next_a = (next_a.astype(F32) + far_a.astype(F32)).astype(BF16)
    prev_b = (prev_b.astype(F32) + far_b.astype(F32)).astype(BF16)
    left_a = turn(next_a, 1)
    right_b = turn(prev_b, -1)
    (leaving,) = call(
        leave_kernel,
        [((experts * packed, 128), BF16)],
        [pltpu.VMEM((experts * packed, 128), F32)],
        own,
        left_a,
        right_a,
        left_b,
        right_b,
    )
    returned = lax.all_to_all(
        leaving.reshape(sources, packed, 128), "sp", split_axis=0, concat_axis=0, tiled=True
    )

    every, passed = gathered(after(grads, next_a, prev_b))
    gate_grad, up_grad = weight_grads(inputs, gate_part, up_part)
    (down_grad,) = call(down_kernel, [((hidden, width), BF16)], [], act_rel, *every)
    returned, gate_grad, up_grad, down_grad = lax.optimization_barrier(
        (returned, gate_grad, up_grad, down_grad)
    )

    core = lax.rem(lax.axis_index("sp"), 2)
    side = share // 2
    mid_grad, sent, kept = call(
        return_kernel,
        [
            ((tok_rows, share), BF16),
            ((groups, side, hidden), BF16),
            ((groups, side, hidden), F32),
        ],
        [pltpu.VMEM((experts * packed, 128), F32)],
        core[None],
        routes.T,
        returned.reshape(experts * packed, 128),
        own_cols,
        gated_all,
    )
    swapped = lax.ppermute(sent, "sp", [(i, i ^ 1) for i in range(sources)])

    mid_left = turn(mid_grad, 1)
    mid_right = turn(mid_grad, -1)
    mid_far = turn(mid_grad, 2)

    paired = (kept + swapped.astype(F32)).astype(BF16)
    chips = sources // 2
    owned = width // sources
    pieces = lax.all_to_all(
        paired.reshape(chips, owned, hidden),
        "sp",
        0,
        0,
        axis_index_groups=[[2 * j + c for j in range(chips)] for c in range(2)],
        tiled=True,
    )
    out_weight_sum = jnp.sum(pieces.astype(F32), axis=0)
    per = chips // groups
    pairs = []
    for j in range(chips):
        for c in range(2):
            for m in range(groups):
                s = (sources // groups) * m + per * c + j % per
                pairs.append(((2 * j + c) * groups + m, s * groups + (m + j // per) % groups))
    out_weight_grad = lax.ppermute(out_weight_sum, ("sp", "tp"), pairs)

    mid_rel = jnp.concatenate([mid_grad, mid_right, mid_far, mid_left], axis=1)
    gated_grad = mm(mid_rel, out_weight_rel, ((1,), (0,)))
    out_gate_grad = (gated_grad * conv).astype(BF16)
    conv_grad = gated_grad * out_gate.astype(F32)
    later = passed_along(conv_grad[:reach], "sp", -1)
    following = jnp.concatenate([conv_grad, later], axis=0)
    mixed_grad = jnp.zeros_like(conv_grad)
    for tap in range(reach + 1):
        mixed_grad = mixed_grad + taps[tap][None, :] * following[tap : tap + tok_rows]
    input_grad = (mixed_grad * in_gate.astype(F32)).astype(BF16)
    in_gate_grad = (mixed_grad * conv_input.astype(F32)).astype(BF16)
    return (
        gate_grad[None],
        up_grad[None],
        down_grad[None],
        mid_grad,
        out_weight_grad,
        input_grad,
        out_gate_grad,
        in_gate_grad,
    )


def solution(mesh):
    in_specs = (
        P("sp", None),
        P("sp", None),
        P("sp", None),
        P(None, "sp", None, None),
        P("sp", None, "tp"),
        P("sp", None, "tp"),
        P("sp", "tp", None),
        P("sp", "tp"),
        P("sp", "tp"),
        P("sp", "tp"),
        P(None, "tp"),
        P(None, "tp"),
    )
    out_specs = (
        P("sp", None, "tp"),
        P("sp", None, "tp"),
        P("sp", "tp", None),
        P("sp", "tp"),
        P("sp", "tp"),
        P("sp", "tp"),
        P("sp", "tp"),
        P("sp", "tp"),
    )

    return jax.shard_map(
        on_device, mesh=mesh, in_specs=in_specs, out_specs=out_specs, check_vma=False
    )
```

```python
import jax
import jax.numpy as jnp
from jax import lax
from jax.experimental import pallas as pl
from jax.experimental.pallas import tpu as pltpu
from jax.sharding import PartitionSpec as P


F32 = jnp.float32
BF16 = jnp.bfloat16


def mm(a, b, contract):
    return lax.dot_general(a, b, ((contract[0], contract[1]), ((), ())), preferred_element_type=F32)


def slot_hits(routes_ref, slots, rows):
    tokens = routes_ref.shape[1]
    row = lax.broadcasted_iota(jnp.int32, (rows, tokens), 0)
    expert = lax.shift_right_logical(row * ((1 << 17) // slots + 1), 17)
    slot = row - expert * slots
    first = routes_ref[0:1, :] == expert
    second = routes_ref[1:2, :] == expert
    named = jnp.where(first | second, 1.0, 0.0)
    sooner = lax.broadcasted_iota(jnp.int32, (tokens, tokens), 0)
    later = lax.broadcasted_iota(jnp.int32, (tokens, tokens), 1)
    order = jnp.where(sooner < later, 1.0, 0.0).astype(BF16)
    place = mm(named.astype(BF16), order, ((1,), (0,)))
    return first, named, place, slot.astype(F32)


def send_kernel(
    first_ref, routes_hbm, weight_hbm, tokens_hbm,
    out_ref, wide_ref, routes_ref, weight_ref, tokens_ref, sems,
):
    loads = [
        pltpu.make_async_copy(routes_hbm, routes_ref, sems.at[0]),
        pltpu.make_async_copy(weight_hbm, weight_ref, sems.at[1]),
        pltpu.make_async_copy(tokens_hbm, tokens_ref, sems.at[2]),
    ]
    for load in loads:
        load.start()
    loads[0].wait()
    loads[1].wait()
    rows = out_ref.shape[0] // (tokens_ref.shape[1] // 128)
    portion = rows // 64
    first, named, place, slot = slot_hits(routes_ref, portion, rows)
    base = first_ref[0].astype(F32)
    hit = jnp.where(place == slot + base, named, 0.0)
    weight = hit * jnp.where(first, weight_ref[0:1, :], weight_ref[1:2, :])
    factor = jnp.sum(weight, axis=1, keepdims=True)
    loads[2].wait()
    picked = mm(hit.astype(BF16), tokens_ref[...], ((1,), (0,))) * factor
    lanes = tokens_ref.shape[1] // 128
    for g in range(lanes):
        wide_ref[pl.ds(g, rows, stride=lanes), :] = picked[:, g * 128 : (g + 1) * 128]
    out_ref[...] = wide_ref[...].astype(BF16)


def arrive_kernel(
    arrived_hbm, w0_hbm, w1_hbm, w2_hbm,
    rows_ref, p0, p1, p2, wide_ref, arrived_ref, w0, w1, w2, sems,
):
    loads = [
        pltpu.make_async_copy(arrived_hbm, arrived_ref, sems.at[0]),
        pltpu.make_async_copy(w2_hbm, w2, sems.at[1]),
        pltpu.make_async_copy(w1_hbm, w1, sems.at[2]),
        pltpu.make_async_copy(w0_hbm, w0, sems.at[3]),
    ]
    for load in loads:
        load.start()
    loads[0].wait()
    wide_ref[...] = arrived_ref[...].astype(F32)
    sources = 64
    per = arrived_ref.shape[0] // sources
    lanes = rows_ref.shape[1] // 128
    for i in range(per // lanes):
        for g in range(lanes):
            rows_ref[i * sources : (i + 1) * sources, g * 128 : (g + 1) * 128] = wide_ref[
                pl.ds(i * lanes + g, sources, stride=per), :
            ].astype(BF16)
    for load, w, p in ((loads[1], w2, p2), (loads[2], w1, p1), (loads[3], w0, p0)):
        load.wait()
        p[...] = mm(rows_ref[...], w[...], ((1,), (1,))).astype(BF16)


def far_kernel(rows_ref, w3a, w3b, p3):
    half = w3a.shape[0]
    p3[:, :half] = mm(rows_ref[...], w3a[...], ((1,), (1,))).astype(BF16)
    p3[:, half:] = mm(rows_ref[...], w3b[...], ((1,), (1,))).astype(BF16)


def row_block(gate_part, up_part, gate_ref, up_ref, which, share):
    span = pl.ds(pl.multiple_of(which * share, share), share)
    block = mm(gate_part, gate_ref[span, :], ((1,), (1,)))
    return block + mm(up_part, up_ref[span, :], ((1,), (1,)))


def parts_kernel(
    member_ref, own, right, far, left, up_of, gate_of, gate_ref, up_ref,
    gate_part, up_part, far_a, far_b,
):
    member = member_ref[0]
    groups = 4
    block = own.shape[0]
    for r, piece in enumerate((own, right, far, left)):
        span = pl.ds(pl.multiple_of(lax.rem(member + r, groups) * block, block), block)
        grad = piece[...].astype(F32)
        up_part[span, :] = (grad * up_of[span, :]).astype(BF16)
        gate_part[span, :] = (grad * gate_of[span, :]).astype(BF16)
    share = far_a.shape[1]
    half = far_a.shape[0]
    which = lax.rem(member + 2, groups)
    part = row_block(gate_part[...], up_part[...], gate_ref, up_ref, which, share).astype(BF16)
    far_a[...] = part[:half]
    far_b[...] = part[half:]


def blocks_kernel(
    member_ref, gate_part, up_part, gate_ref, up_ref,
    next_a, next_b, prev_a, prev_b, own,
):
    member = member_ref[0]
    half, share = next_a.shape
    for by, a, b in ((1, next_a, next_b), (3, prev_a, prev_b)):
        which = lax.rem(member + by, 4)
        part = row_block(gate_part[...], up_part[...], gate_ref, up_ref, which, share)
        a[...] = part[:half].astype(BF16)
        b[...] = part[half:].astype(BF16)
    own[...] = row_block(gate_part[...], up_part[...], gate_ref, up_ref, member, share)


def leave_kernel(own, left_a, right_a, left_b, right_b, out_ref, wide_ref):
    sources = 64
    half, share = left_a.shape
    lanes = share // 128
    per = out_ref.shape[0] // sources
    for p in range(per // lanes):
        left, right = (left_a, right_a) if p * sources < half else (left_b, right_b)
        at = p * sources
        here = at if at < half else at - half
        rows = own[at : at + sources, :]
        rows = rows + left[here : here + sources, :].astype(F32)
        rows = rows + right[here : here + sources, :].astype(F32)
        for g in range(lanes):
            wide_ref[pl.ds(p * lanes + g, sources, stride=per), :] = rows[
                :, g * 128 : (g + 1) * 128
            ]
    out_ref[...] = wide_ref[...].astype(BF16)


def return_kernel(
    where_ref, routes_ref, returned_ref, tokens_hbm, gated_ref,
    mid_ref, sent_ref, kept_ref, wide_ref, own_ref, sem,
):
    share = mid_ref.shape[1]
    first = pl.multiple_of(where_ref[0] * share, share)
    load = pltpu.make_async_copy(tokens_hbm.at[:, pl.ds(first, share)], own_ref, sem)
    load.start()
    lanes = share // 128
    columns = returned_ref.shape[0] // lanes
    wide_ref[...] = returned_ref[...].astype(F32)
    _, named, place, slot = slot_hits(routes_ref, columns // 64, columns)
    hit = jnp.where(place == slot, named, 0.0).T.astype(BF16)
    load.wait()
    for g in range(lanes):
        rows = wide_ref[pl.ds(g, columns, stride=lanes), :].astype(BF16)
        picked = mm(hit, rows, ((1,), (0,)))
        own = own_ref[:, g * 128 : (g + 1) * 128].astype(F32)
        mid_ref[:, g * 128 : (g + 1) * 128] = (own + picked).astype(BF16)
    side = share // 2
    core = where_ref[1]
    for ref, which in ((sent_ref, 1 - core), (kept_ref, core)):
        columns_t = mid_ref[:, pl.ds(pl.multiple_of(which * side, side), side)].T
        for r in range(gated_ref.shape[0]):
            part = mm(columns_t, gated_ref[r], ((1,), (0,)))
            ref[r] = part.astype(ref.dtype)


def down_kernel(member_ref, act, g0, g1, g2, g3a, g3b, out_ref):
    half = g3a.shape[0]

    def block(by):
        return act[lax.rem(member_ref[0] + by, 4)]

    total = mm(block(0).T, g0[...], ((1,), (0,)))
    total = total + mm(block(3).T, g1[...], ((1,), (0,)))
    total = total + mm(block(1).T, g2[...], ((1,), (0,)))
    far = block(2)
    total = total + mm(far[:half].T, g3a[...], ((1,), (0,)))
    total = total + mm(far[half:].T, g3b[...], ((1,), (0,)))
    out_ref[...] = total.astype(BF16)


def halves_kernel(left, right, a, b, sems):
    half = a.shape[0]
    copies = [
        pltpu.make_async_copy(left.at[pl.ds(0, half), :], a, sems.at[0]),
        pltpu.make_async_copy(right.at[pl.ds(half, half), :], b, sems.at[1]),
    ]
    for copy in copies:
        copy.start()
    for copy in copies:
        copy.wait()


def weights_kernel(x_ref, gate_part, up_part, gate_ref, up_ref):
    x = x_ref[...].T
    gate_ref[...] = mm(x, gate_part[...], ((1,), (0,))).astype(BF16)
    up_ref[...] = mm(x, up_part[...], ((1,), (0,))).astype(BF16)


def weight_grads(inputs, gate_part, up_part):
    rows, width = inputs.shape
    hidden = gate_part.shape[1]
    tile = 512
    whole = pl.BlockSpec((rows, hidden), lambda i: (0, 0))
    out = pl.BlockSpec((tile, hidden), lambda i: (i, 0))
    return pl.pallas_call(
        weights_kernel,
        grid=(width // tile,),
        out_shape=[jax.ShapeDtypeStruct((width, hidden), BF16)] * 2,
        in_specs=[pl.BlockSpec((rows, tile), lambda i: (0, i)), whole, whole],
        out_specs=[out, out],
        compiler_params=pltpu.CompilerParams(vmem_limit_bytes=40 << 20),
        name="weights",
    )(inputs, gate_part, up_part)


def call(kernel, outs, scratch, *args, there=(), limit=40 << 20):
    smem = pl.BlockSpec(memory_space=pltpu.SMEM)
    vmem = pl.BlockSpec(memory_space=pltpu.VMEM)
    hbm = pl.BlockSpec(memory_space=pltpu.HBM)
    return pl.pallas_call(
        kernel,
        out_shape=[jax.ShapeDtypeStruct(*o) for o in outs],
        in_specs=[smem if a.ndim == 1 else hbm if i in there else vmem for i, a in enumerate(args)],
        out_specs=[vmem] * len(outs),
        scratch_shapes=scratch,
        compiler_params=pltpu.CompilerParams(vmem_limit_bytes=limit),
    )(*args)


def turn(shard, by):
    peers = lax.axis_size("tp")
    return lax.ppermute(shard, "tp", [(i, (i + by) % peers) for i in range(peers)])


def passed_along(shard, axis, by):
    peers = lax.axis_size(axis)
    pairs = [(i, i + by) for i in range(peers) if 0 <= i + by < peers]
    return lax.ppermute(shard, axis, pairs)


def after(value, *others):
    return lax.optimization_barrier((value, *others))[0]


def gathered(own, *earlier):
    left = turn(own, 1)
    right = turn(own, -1)
    left, right, *earlier = lax.optimization_barrier((left, right, *earlier))
    half = (own.shape[0] // 2, own.shape[1])
    passed_a, passed_b = call(
        halves_kernel,
        [(half, own.dtype)] * 2,
        [pltpu.SemaphoreType.DMA((2,))],
        left,
        right,
        there=(0, 1),
        limit=4 << 20,
    )
    far_a = turn(passed_a, 1)
    far_b = turn(passed_b, -1)
    return (own, left, right, far_a, far_b), (passed_a, passed_b), earlier


def on_device(
    out_grad,
    routes,
    route_weight,
    expert_rows,
    gate_weight,
    up_weight,
    down_weight,
    conv_input,
    out_gate,
    in_gate,
    taps,
    out_weight,
):
    groups = lax.axis_size("tp")
    member = lax.axis_index("tp")
    sources = lax.axis_size("sp")
    tok_rows, width = out_grad.shape
    slots = expert_rows.shape[2]
    share = width // groups
    portion = slots // groups
    experts = sources
    hidden = gate_weight.shape[2]
    rows = slots * sources


    packed = portion * width // 128
    (piece,) = call(
        send_kernel,
        [((experts * packed, 128), BF16)],
        [
            pltpu.VMEM((experts * packed, 128), F32),
            pltpu.VMEM(routes.T.shape, jnp.int32),
            pltpu.VMEM(routes.T.shape, F32),
            pltpu.VMEM(out_grad.shape, BF16),
            pltpu.SemaphoreType.DMA((3,)),
        ],
        (member * portion)[None],
        routes.T,
        route_weight.T,
        out_grad,
        there=(1, 2, 3),
        limit=67_000_000,
    )
    arrived = lax.all_to_all(
        piece.reshape(experts, packed, 128), "sp", split_axis=0, concat_axis=0, tiled=True
    )

    out_weight_twice = after(out_weight, piece)
    out_weight_twice = jnp.concatenate([out_weight_twice, out_weight_twice], axis=0)
    out_weight_rel = lax.dynamic_slice_in_dim(out_weight_twice, member * share, width, 0)
    w_down, passed, (out_weight_rel,) = gathered(down_weight[0], out_weight_rel)

    inputs = expert_rows[:, 0].transpose(1, 0, 2).reshape(rows, width)
    inputs = after(inputs, *passed)
    gate_w, up_w = gate_weight[0], up_weight[0]
    gate = mm(inputs, gate_w, ((1,), (0,)))
    up = mm(inputs, up_w, ((1,), (0,)))
    sig = jax.nn.sigmoid(gate)
    act = (gate * sig * up).astype(BF16)
    up_of = gate * sig
    gate_of = up * sig * (1.0 + gate * (1.0 - sig))
    act = act.reshape(groups, rows // groups, hidden)
    (
        arrived, up_of, gate_of, act, out_weight_rel
    ) = lax.optimization_barrier(
        (arrived, up_of, gate_of, act, out_weight_rel)
    )

    block = portion * sources
    grads, *partial = call(
        arrive_kernel,
        [((block, width), BF16)] + [((block, hidden), BF16)] * 3,
        [
            pltpu.VMEM((sources * packed, 128), F32),
            pltpu.VMEM((sources * packed, 128), BF16),
            *[pltpu.VMEM((hidden, width), BF16)] * 3,
            pltpu.SemaphoreType.DMA((4,)),
        ],
        arrived.reshape(sources * packed, 128),
        *w_down[:3],
        there=(0, 1, 2, 3),
        limit=65_200_000,
    )
    from_left = turn(partial[2], 1)
    from_right = turn(partial[1], -1)
    (partial_far,) = call(far_kernel, [((block, hidden), BF16)], [], grads, w_down[3], w_down[4])
    from_far = turn(partial_far, 2)
    half = rows // 2
    gate_part, up_part, far_a, far_b = call(
        parts_kernel,
        [((rows, hidden), BF16)] * 2 + [((half, share), BF16)] * 2,
        [],
        member[None],
        partial[0],
        from_right,
        from_far,
        from_left,
        up_of,
        gate_of,
        gate_w,
        up_w,
    )
    far_a = turn(far_a, 1)
    far_b = turn(far_b, -1)
    next_a, next_b, prev_a, prev_b, own = call(
        blocks_kernel,
        [((half, share), BF16)] * 4 + [((rows, share), F32)],
        [],
        member[None],
        gate_part,
        up_part,
        gate_w,
        up_w,
    )
    left_b = turn(next_b, 1)
    right_a = turn(prev_a, -1)
    next_a = (next_a.astype(F32) + far_a.astype(F32)).astype(BF16)
    prev_b = (prev_b.astype(F32) + far_b.astype(F32)).astype(BF16)
    left_a = turn(next_a, 1)
    right_b = turn(prev_b, -1)

    in_gate, conv_input, out_gate = lax.optimization_barrier(
        (in_gate, conv_input, out_gate, next_a, prev_b)
    )[:3]
    reach = taps.shape[0] - 1
    mixed = in_gate.astype(F32) * conv_input.astype(F32)
    prior_mixed = passed_along(mixed[tok_rows - reach :], "sp", 1)
    extended = jnp.concatenate([prior_mixed, mixed], axis=0)
    conv = jnp.zeros_like(mixed)
    for tap in range(reach + 1):
        conv = conv + taps[tap][None, :] * extended[reach - tap : reach - tap + tok_rows]
    gated = (out_gate.astype(F32) * conv).astype(BF16)
    gate_grad, up_grad = weight_grads(inputs, gate_part, up_part)
    left_a, right_b, conv, gated, gate_grad, up_grad = lax.optimization_barrier(
        (left_a, right_b, conv, gated, gate_grad, up_grad)
    )
    (leaving,) = call(
        leave_kernel,
        [((experts * packed, 128), BF16)],
        [pltpu.VMEM((experts * packed, 128), F32)],
        own,
        left_a,
        right_a,
        left_b,
        right_b,
    )
    returned = lax.all_to_all(
        leaving.reshape(sources, packed, 128), "sp", split_axis=0, concat_axis=0, tiled=True
    )

    every, passed, _ = gathered(after(grads, next_a, prev_b))
    gated = after(gated, leaving)
    gated_right = turn(gated, -1)
    gated_far = turn(gated, 2)
    gated_left = turn(gated, 1)
    gated_all = jnp.stack([gated, gated_right, gated_far, gated_left])
    (down_grad,) = call(down_kernel, [((hidden, width), BF16)], [], member[None], act, *every)
    returned, gated_all = lax.optimization_barrier((returned, gated_all))

    core = lax.rem(lax.axis_index("sp"), 2)
    side = share // 2
    mid_grad, sent, kept = call(
        return_kernel,
        [
            ((tok_rows, share), BF16),
            ((groups, side, hidden), BF16),
            ((groups, side, hidden), F32),
        ],
        [
            pltpu.VMEM((experts * packed, 128), F32),
            pltpu.VMEM((tok_rows, share), BF16),
            pltpu.SemaphoreType.DMA,
        ],
        jnp.stack([member, core]),
        routes.T,
        returned.reshape(experts * packed, 128),
        out_grad,
        gated_all,
        there=(3,),
    )
    swapped = lax.ppermute(sent, "sp", [(i, i ^ 1) for i in range(sources)])

    mid_left = turn(mid_grad, 1)
    mid_right = turn(mid_grad, -1)
    mid_far = turn(mid_grad, 2)

    paired = (kept + swapped.astype(F32)).astype(BF16)
    chips = sources // 2
    owned = width // sources
    pieces = lax.all_to_all(
        paired.reshape(chips, owned, hidden),
        "sp",
        0,
        0,
        axis_index_groups=[[2 * j + c for j in range(chips)] for c in range(2)],
        tiled=True,
    )
    out_weight_sum = jnp.sum(pieces.astype(F32), axis=0)
    per = chips // groups
    pairs = []
    for j in range(chips):
        for c in range(2):
            for m in range(groups):
                s = (sources // groups) * m + per * c + j % per
                pairs.append(((2 * j + c) * groups + m, s * groups + (m + j // per) % groups))
    out_weight_grad = lax.ppermute(out_weight_sum, ("sp", "tp"), pairs)

    mid_rel = jnp.concatenate([mid_grad, mid_right, mid_far, mid_left], axis=1)
    gated_grad = mm(mid_rel, out_weight_rel, ((1,), (0,)))
    out_gate_grad = (gated_grad * conv).astype(BF16)
    conv_grad = gated_grad * out_gate.astype(F32)
    later = passed_along(conv_grad[:reach], "sp", -1)
    following = jnp.concatenate([conv_grad, later], axis=0)
    mixed_grad = jnp.zeros_like(conv_grad)
    for tap in range(reach + 1):
        mixed_grad = mixed_grad + taps[tap][None, :] * following[tap : tap + tok_rows]
    input_grad = (mixed_grad * in_gate.astype(F32)).astype(BF16)
    in_gate_grad = (mixed_grad * conv_input.astype(F32)).astype(BF16)
    return (
        gate_grad[None],
        up_grad[None],
        down_grad[None],
        mid_grad,
        out_weight_grad,
        input_grad,
        out_gate_grad,
        in_gate_grad,
    )


def solution(mesh):
    in_specs = (
        P("sp", None),
        P("sp", None),
        P("sp", None),
        P(None, "sp", None, None),
        P("sp", None, "tp"),
        P("sp", None, "tp"),
        P("sp", "tp", None),
        P("sp", "tp"),
        P("sp", "tp"),
        P("sp", "tp"),
        P(None, "tp"),
        P(None, "tp"),
    )
    out_specs = (
        P("sp", None, "tp"),
        P("sp", None, "tp"),
        P("sp", "tp", None),
        P("sp", "tp"),
        P("sp", "tp"),
        P("sp", "tp"),
        P("sp", "tp"),
        P("sp", "tp"),
    )

    return jax.shard_map(
        on_device, mesh=mesh, in_specs=in_specs, out_specs=out_specs, check_vma=False
    )
```

```python
import jax
import jax.numpy as jnp
from jax import lax
from jax.experimental import pallas as pl
from jax.experimental.pallas import tpu as pltpu
from jax.sharding import PartitionSpec as P


F32 = jnp.float32
BF16 = jnp.bfloat16


STEPS = ((5, 4), (7, 2), (0, 1), (6, 3))


def mm(a, b, contract):
    return lax.dot_general(a, b, ((contract[0], contract[1]), ((), ())), preferred_element_type=F32)


def slot_hits(routes_ref, slots, rows):
    tokens = routes_ref.shape[1]
    row = lax.broadcasted_iota(jnp.int32, (rows, tokens), 0)
    expert = lax.shift_right_logical(row * ((1 << 17) // slots + 1), 17)
    slot = row - expert * slots
    first = routes_ref[0:1, :] == expert
    second = routes_ref[1:2, :] == expert
    named = jnp.where(first | second, 1.0, 0.0)
    sooner = lax.broadcasted_iota(jnp.int32, (tokens, tokens), 0)
    later = lax.broadcasted_iota(jnp.int32, (tokens, tokens), 1)
    order = jnp.where(sooner < later, 1.0, 0.0).astype(BF16)
    place = mm(named.astype(BF16), order, ((1,), (0,)))
    return first, named, place, slot.astype(F32)


def send_kernel(
    first_ref, routes_hbm, weight_hbm, tokens_hbm,
    out_ref, wide_ref, routes_ref, weight_ref, tokens_ref, sems,
):
    loads = [
        pltpu.make_async_copy(routes_hbm, routes_ref, sems.at[0]),
        pltpu.make_async_copy(weight_hbm, weight_ref, sems.at[1]),
        pltpu.make_async_copy(tokens_hbm, tokens_ref, sems.at[2]),
    ]
    for load in loads:
        load.start()
    loads[0].wait()
    loads[1].wait()
    rows = out_ref.shape[0] // (tokens_ref.shape[1] // 128)
    portion = rows // 64
    first, named, place, slot = slot_hits(routes_ref, portion, rows)
    base = first_ref[0].astype(F32)
    hit = jnp.where(place == slot + base, named, 0.0)
    weight = hit * jnp.where(first, weight_ref[0:1, :], weight_ref[1:2, :])
    factor = jnp.sum(weight, axis=1, keepdims=True)
    loads[2].wait()
    picked = mm(hit.astype(BF16), tokens_ref[...], ((1,), (0,))) * factor
    lanes = tokens_ref.shape[1] // 128
    for g in range(lanes):
        wide_ref[pl.ds(g, rows, stride=lanes), :] = picked[:, g * 128 : (g + 1) * 128]
    out_ref[...] = wide_ref[...].astype(BF16)


def arrive_kernel(
    arrived_hbm, w0_hbm, w1_hbm, w2_hbm,
    rows_ref, p0, p1, p2, wide_ref, arrived_ref, w0, w1, w2, sems,
):
    loads = [
        pltpu.make_async_copy(arrived_hbm, arrived_ref, sems.at[0]),
        pltpu.make_async_copy(w2_hbm, w2, sems.at[1]),
        pltpu.make_async_copy(w1_hbm, w1, sems.at[2]),
        pltpu.make_async_copy(w0_hbm, w0, sems.at[3]),
    ]
    for load in loads:
        load.start()
    loads[0].wait()
    wide_ref[...] = arrived_ref[...].astype(F32)
    sources = 64
    per = arrived_ref.shape[0] // sources
    lanes = rows_ref.shape[1] // 128
    for i in range(per // lanes):
        for g in range(lanes):
            rows_ref[i * sources : (i + 1) * sources, g * 128 : (g + 1) * 128] = wide_ref[
                pl.ds(i * lanes + g, sources, stride=per), :
            ].astype(BF16)
    for load, w, p in ((loads[1], w2, p2), (loads[2], w1, p1), (loads[3], w0, p0)):
        load.wait()
        p[...] = mm(rows_ref[...], w[...], ((1,), (1,))).astype(BF16)


def far_kernel(rows_ref, w3a, w3b, p3):
    half = w3a.shape[0]
    p3[:, :half] = mm(rows_ref[...], w3a[...], ((1,), (1,))).astype(BF16)
    p3[:, half:] = mm(rows_ref[...], w3b[...], ((1,), (1,))).astype(BF16)


def row_block(gate_part, up_part, gate_ref, up_ref, which, share):
    span = pl.ds(pl.multiple_of(which * share, share), share)
    block = mm(gate_part, gate_ref[span, :], ((1,), (1,)))
    return block + mm(up_part, up_ref[span, :], ((1,), (1,)))


def parts_kernel(
    member_ref, own, right, far, left, up_of, gate_of, gate_ref, up_ref,
    gate_part, up_part, far_a, far_b,
):
    member = member_ref[0]
    groups = 4
    block = own.shape[0]
    for r, piece in enumerate((own, right, far, left)):
        span = pl.ds(pl.multiple_of(lax.rem(member + r, groups) * block, block), block)
        grad = piece[...].astype(F32)
        up_part[span, :] = (grad * up_of[span, :]).astype(BF16)
        gate_part[span, :] = (grad * gate_of[span, :]).astype(BF16)
    share = far_a.shape[1]
    half = far_a.shape[0]
    which = lax.rem(member + 2, groups)
    part = row_block(gate_part[...], up_part[...], gate_ref, up_ref, which, share).astype(BF16)
    far_a[...] = part[:half]
    far_b[...] = part[half:]


def blocks_kernel(
    member_ref, gate_part, up_part, gate_ref, up_ref,
    next_a, next_b, prev_a, prev_b, own,
):
    member = member_ref[0]
    half, share = next_a.shape
    for by, a, b in ((1, next_a, next_b), (3, prev_a, prev_b)):
        which = lax.rem(member + by, 4)
        part = row_block(gate_part[...], up_part[...], gate_ref, up_ref, which, share)
        a[...] = part[:half].astype(BF16)
        b[...] = part[half:].astype(BF16)
    own[...] = row_block(gate_part[...], up_part[...], gate_ref, up_ref, member, share)


def leave_kernel(own, left_a, right_a, left_b, right_b, out_ref, wide_ref):
    sources = 64
    half, share = left_a.shape
    lanes = share // 128
    per = out_ref.shape[0] // sources
    for p in range(per // lanes):
        left, right = (left_a, right_a) if p * sources < half else (left_b, right_b)
        at = p * sources
        here = at if at < half else at - half
        rows = own[at : at + sources, :]
        rows = rows + left[here : here + sources, :].astype(F32)
        rows = rows + right[here : here + sources, :].astype(F32)
        for g in range(lanes):
            wide_ref[pl.ds(p * lanes + g, sources, stride=per), :] = rows[
                :, g * 128 : (g + 1) * 128
            ]
    out_ref[...] = wide_ref[...].astype(BF16)


def return_kernel(
    where_ref, routes_ref, returned_ref, tokens_hbm, gated_ref,
    mid_ref, sent_ref, kept_ref, wide_ref, own_ref, sem,
):
    share = mid_ref.shape[1]
    first = pl.multiple_of(where_ref[0] * share, share)
    load = pltpu.make_async_copy(tokens_hbm.at[:, pl.ds(first, share)], own_ref, sem)
    load.start()
    lanes = share // 128
    columns = returned_ref.shape[0] // lanes
    wide_ref[...] = returned_ref[...].astype(F32)
    _, named, place, slot = slot_hits(routes_ref, columns // 64, columns)
    hit = jnp.where(place == slot, named, 0.0).T.astype(BF16)
    load.wait()
    for g in range(lanes):
        rows = wide_ref[pl.ds(g, columns, stride=lanes), :].astype(BF16)
        picked = mm(hit, rows, ((1,), (0,)))
        own = own_ref[:, g * 128 : (g + 1) * 128].astype(F32)
        mid_ref[:, g * 128 : (g + 1) * 128] = (own + picked).astype(BF16)
    side = share // 2
    core = where_ref[1]
    for ref, which in ((sent_ref, 1 - core), (kept_ref, core)):
        columns_t = mid_ref[:, pl.ds(pl.multiple_of(which * side, side), side)].T
        owned = ref.shape[1]
        for r in range(gated_ref.shape[0]):
            part = mm(columns_t, gated_ref[r], ((1,), (0,))).astype(ref.dtype)
            for k in range(side // owned):
                z = lax.rem(2 * where_ref[0] + which + STEPS[r][k % 2], 8)
                ref[z * 4 + k // 2] = part[k * owned : (k + 1) * owned]


def down_kernel(member_ref, act, g0, g1, g2, g3a, g3b, out_ref):
    half = g3a.shape[0]

    def block(by):
        return act[lax.rem(member_ref[0] + by, 4)]

    total = mm(block(0).T, g0[...], ((1,), (0,)))
    total = total + mm(block(3).T, g1[...], ((1,), (0,)))
    total = total + mm(block(1).T, g2[...], ((1,), (0,)))
    far = block(2)
    total = total + mm(far[:half].T, g3a[...], ((1,), (0,)))
    total = total + mm(far[half:].T, g3b[...], ((1,), (0,)))
    out_ref[...] = total.astype(BF16)


def halves_kernel(left, right, a, b, sems):
    half = a.shape[0]
    copies = [
        pltpu.make_async_copy(left.at[pl.ds(0, half), :], a, sems.at[0]),
        pltpu.make_async_copy(right.at[pl.ds(half, half), :], b, sems.at[1]),
    ]
    for copy in copies:
        copy.start()
    for copy in copies:
        copy.wait()


def weights_kernel(x_ref, gate_part, up_part, gate_ref, up_ref):
    x = x_ref[...].T
    gate_ref[...] = mm(x, gate_part[...], ((1,), (0,))).astype(BF16)
    up_ref[...] = mm(x, up_part[...], ((1,), (0,))).astype(BF16)


def weight_grads(inputs, gate_part, up_part):
    rows, width = inputs.shape
    hidden = gate_part.shape[1]
    tile = 512
    whole = pl.BlockSpec((rows, hidden), lambda i: (0, 0))
    out = pl.BlockSpec((tile, hidden), lambda i: (i, 0))
    return pl.pallas_call(
        weights_kernel,
        grid=(width // tile,),
        out_shape=[jax.ShapeDtypeStruct((width, hidden), BF16)] * 2,
        in_specs=[pl.BlockSpec((rows, tile), lambda i: (0, i)), whole, whole],
        out_specs=[out, out],
        compiler_params=pltpu.CompilerParams(vmem_limit_bytes=40 << 20),
        name="weights",
    )(inputs, gate_part, up_part)


def call(kernel, outs, scratch, *args, there=(), limit=40 << 20):
    smem = pl.BlockSpec(memory_space=pltpu.SMEM)
    vmem = pl.BlockSpec(memory_space=pltpu.VMEM)
    hbm = pl.BlockSpec(memory_space=pltpu.HBM)
    return pl.pallas_call(
        kernel,
        out_shape=[jax.ShapeDtypeStruct(*o) for o in outs],
        in_specs=[smem if a.ndim == 1 else hbm if i in there else vmem for i, a in enumerate(args)],
        out_specs=[vmem] * len(outs),
        scratch_shapes=scratch,
        compiler_params=pltpu.CompilerParams(vmem_limit_bytes=limit),
    )(*args)


def turn(shard, by):
    peers = lax.axis_size("tp")
    return lax.ppermute(shard, "tp", [(i, (i + by) % peers) for i in range(peers)])


def passed_along(shard, axis, by):
    peers = lax.axis_size(axis)
    pairs = [(i, i + by) for i in range(peers) if 0 <= i + by < peers]
    return lax.ppermute(shard, axis, pairs)


def after(value, *others):
    return lax.optimization_barrier((value, *others))[0]


def gathered(own, *earlier):
    left = turn(own, 1)
    right = turn(own, -1)
    left, right, *earlier = lax.optimization_barrier((left, right, *earlier))
    half = (own.shape[0] // 2, own.shape[1])
    passed_a, passed_b = call(
        halves_kernel,
        [(half, own.dtype)] * 2,
        [pltpu.SemaphoreType.DMA((2,))],
        left,
        right,
        there=(0, 1),
        limit=4 << 20,
    )
    far_a = turn(passed_a, 1)
    far_b = turn(passed_b, -1)
    return (own, left, right, far_a, far_b), (passed_a, passed_b), earlier


def on_device(
    out_grad,
    routes,
    route_weight,
    expert_rows,
    gate_weight,
    up_weight,
    down_weight,
    conv_input,
    out_gate,
    in_gate,
    taps,
    out_weight,
):
    groups = lax.axis_size("tp")
    member = lax.axis_index("tp")
    sources = lax.axis_size("sp")
    tok_rows, width = out_grad.shape
    slots = expert_rows.shape[2]
    share = width // groups
    portion = slots // groups
    experts = sources
    hidden = gate_weight.shape[2]
    rows = slots * sources


    packed = portion * width // 128
    (piece,) = call(
        send_kernel,
        [((experts * packed, 128), BF16)],
        [
            pltpu.VMEM((experts * packed, 128), F32),
            pltpu.VMEM(routes.T.shape, jnp.int32),
            pltpu.VMEM(routes.T.shape, F32),
            pltpu.VMEM(out_grad.shape, BF16),
            pltpu.SemaphoreType.DMA((3,)),
        ],
        (member * portion)[None],
        routes.T,
        route_weight.T,
        out_grad,
        there=(1, 2, 3),
        limit=67_000_000,
    )
    arrived = lax.all_to_all(
        piece.reshape(experts, packed, 128), "sp", split_axis=0, concat_axis=0, tiled=True
    )

    out_weight_twice = after(out_weight, piece)
    out_weight_twice = jnp.concatenate([out_weight_twice, out_weight_twice], axis=0)
    out_weight_rel = lax.dynamic_slice_in_dim(out_weight_twice, member * share, width, 0)
    w_down, passed, (out_weight_rel,) = gathered(down_weight[0], out_weight_rel)

    inputs = expert_rows[:, 0].transpose(1, 0, 2).reshape(rows, width)
    inputs = after(inputs, *passed)
    gate_w, up_w = gate_weight[0], up_weight[0]
    gate = mm(inputs, gate_w, ((1,), (0,)))
    up = mm(inputs, up_w, ((1,), (0,)))
    sig = jax.nn.sigmoid(gate)
    act = (gate * sig * up).astype(BF16)
    up_of = gate * sig
    gate_of = up * sig * (1.0 + gate * (1.0 - sig))
    act = act.reshape(groups, rows // groups, hidden)
    (
        arrived, up_of, gate_of, act, out_weight_rel
    ) = lax.optimization_barrier(
        (arrived, up_of, gate_of, act, out_weight_rel)
    )

    block = portion * sources
    grads, *partial = call(
        arrive_kernel,
        [((block, width), BF16)] + [((block, hidden), BF16)] * 3,
        [
            pltpu.VMEM((sources * packed, 128), F32),
            pltpu.VMEM((sources * packed, 128), BF16),
            *[pltpu.VMEM((hidden, width), BF16)] * 3,
            pltpu.SemaphoreType.DMA((4,)),
        ],
        arrived.reshape(sources * packed, 128),
        *w_down[:3],
        there=(0, 1, 2, 3),
        limit=65_200_000,
    )
    from_left = turn(partial[2], 1)
    from_right = turn(partial[1], -1)
    (partial_far,) = call(far_kernel, [((block, hidden), BF16)], [], grads, w_down[3], w_down[4])
    from_far = turn(partial_far, 2)
    half = rows // 2
    gate_part, up_part, far_a, far_b = call(
        parts_kernel,
        [((rows, hidden), BF16)] * 2 + [((half, share), BF16)] * 2,
        [],
        member[None],
        partial[0],
        from_right,
        from_far,
        from_left,
        up_of,
        gate_of,
        gate_w,
        up_w,
    )
    far_a = turn(far_a, 1)
    far_b = turn(far_b, -1)
    next_a, next_b, prev_a, prev_b, own = call(
        blocks_kernel,
        [((half, share), BF16)] * 4 + [((rows, share), F32)],
        [],
        member[None],
        gate_part,
        up_part,
        gate_w,
        up_w,
    )
    left_b = turn(next_b, 1)
    right_a = turn(prev_a, -1)
    next_a = (next_a.astype(F32) + far_a.astype(F32)).astype(BF16)
    prev_b = (prev_b.astype(F32) + far_b.astype(F32)).astype(BF16)
    left_a = turn(next_a, 1)
    right_b = turn(prev_b, -1)

    in_gate, conv_input, out_gate = lax.optimization_barrier(
        (in_gate, conv_input, out_gate, next_a, prev_b)
    )[:3]
    reach = taps.shape[0] - 1
    mixed = in_gate.astype(F32) * conv_input.astype(F32)
    prior_mixed = passed_along(mixed[tok_rows - reach :], "sp", 1)
    extended = jnp.concatenate([prior_mixed, mixed], axis=0)
    conv = jnp.zeros_like(mixed)
    for tap in range(reach + 1):
        conv = conv + taps[tap][None, :] * extended[reach - tap : reach - tap + tok_rows]
    gated = (out_gate.astype(F32) * conv).astype(BF16)
    gate_grad, up_grad = weight_grads(inputs, gate_part, up_part)
    left_a, right_b, conv, gated, gate_grad, up_grad = lax.optimization_barrier(
        (left_a, right_b, conv, gated, gate_grad, up_grad)
    )
    (leaving,) = call(
        leave_kernel,
        [((experts * packed, 128), BF16)],
        [pltpu.VMEM((experts * packed, 128), F32)],
        own,
        left_a,
        right_a,
        left_b,
        right_b,
    )
    returned = lax.all_to_all(
        leaving.reshape(sources, packed, 128), "sp", split_axis=0, concat_axis=0, tiled=True
    )

    every, passed, _ = gathered(after(grads, next_a, prev_b))
    gated = after(gated, leaving)
    gated_right = turn(gated, -1)
    gated_far = turn(gated, 2)
    gated_left = turn(gated, 1)
    gated_all = jnp.stack([gated, gated_right, gated_far, gated_left])
    (down_grad,) = call(down_kernel, [((hidden, width), BF16)], [], member[None], act, *every)
    returned, gated_all = lax.optimization_barrier((returned, gated_all))

    core = lax.rem(lax.axis_index("sp"), 2)
    mid_grad, sent, kept = call(
        return_kernel,
        [
            ((tok_rows, share), BF16),
            ((sources // 2, width // sources, hidden), BF16),
            ((sources // 2, width // sources, hidden), F32),
        ],
        [
            pltpu.VMEM((experts * packed, 128), F32),
            pltpu.VMEM((tok_rows, share), BF16),
            pltpu.SemaphoreType.DMA,
        ],
        jnp.stack([member, core]),
        routes.T,
        returned.reshape(experts * packed, 128),
        out_grad,
        gated_all,
        there=(3,),
    )
    swapped = lax.ppermute(sent, "sp", [(i, i ^ 1) for i in range(sources)])

    mid_left = turn(mid_grad, 1)
    mid_right = turn(mid_grad, -1)
    mid_far = turn(mid_grad, 2)

    paired = (kept + swapped.astype(F32)).astype(BF16)
    chips = sources // 2
    pieces = lax.all_to_all(
        paired,
        "sp",
        0,
        0,
        axis_index_groups=[[2 * j + c for j in range(chips)] for c in range(2)],
        tiled=True,
    )
    out_weight_sum = jnp.sum(pieces.astype(F32), axis=0)
    pairs = []
    for z in range(8):
        for y in range(4):
            for c in range(2):
                for m in range(groups):
                    step = (z - 2 * m - c) % 8
                    r, k = next((r, k) for r in range(4) for k in range(2) if STEPS[r][k] == step)
                    here = (z * 4 + y) * 2 + c
                    owner = 16 * m + 8 * c + 2 * y + k
                    pairs.append((here * groups + m, owner * groups + (m + r) % groups))
    out_weight_grad = lax.ppermute(out_weight_sum, ("sp", "tp"), pairs)

    mid_rel = jnp.concatenate([mid_grad, mid_right, mid_far, mid_left], axis=1)
    gated_grad = mm(mid_rel, out_weight_rel, ((1,), (0,)))
    out_gate_grad = (gated_grad * conv).astype(BF16)
    conv_grad = gated_grad * out_gate.astype(F32)
    later = passed_along(conv_grad[:reach], "sp", -1)
    following = jnp.concatenate([conv_grad, later], axis=0)
    mixed_grad = jnp.zeros_like(conv_grad)
    for tap in range(reach + 1):
        mixed_grad = mixed_grad + taps[tap][None, :] * following[tap : tap + tok_rows]
    input_grad = (mixed_grad * in_gate.astype(F32)).astype(BF16)
    in_gate_grad = (mixed_grad * conv_input.astype(F32)).astype(BF16)
    return (
        gate_grad[None],
        up_grad[None],
        down_grad[None],
        mid_grad,
        out_weight_grad,
        input_grad,
        out_gate_grad,
        in_gate_grad,
    )


def solution(mesh):
    in_specs = (
        P("sp", None),
        P("sp", None),
        P("sp", None),
        P(None, "sp", None, None),
        P("sp", None, "tp"),
        P("sp", None, "tp"),
        P("sp", "tp", None),
        P("sp", "tp"),
        P("sp", "tp"),
        P("sp", "tp"),
        P(None, "tp"),
        P(None, "tp"),
    )
    out_specs = (
        P("sp", None, "tp"),
        P("sp", None, "tp"),
        P("sp", "tp", None),
        P("sp", "tp"),
        P("sp", "tp"),
        P("sp", "tp"),
        P("sp", "tp"),
        P("sp", "tp"),
    )

    return jax.shard_map(
        on_device, mesh=mesh, in_specs=in_specs, out_specs=out_specs, check_vma=False
    )
```
